32 devices in a mesh: sp: 8 (over z, x), tp: 4 (over y, core).
Axes of the slice: x: 2, y: 2, z: 4, core: 2. Of those that a mesh axis runs over, the one named last changes fastest.
Arguments:
- query_rows: bfloat16 [4096, 1024], P('sp', 'tp'), may hold values from -6 to 6
- key_rows: bfloat16 [4096, 1024], P('sp', 'tp'), may hold values from -6 to 6
- value_rows: bfloat16 [4096, 2048], P('sp', 'tp'), may hold values from -6 to 6
- out_gate_pre: bfloat16 [4096, 2048], P('sp', 'tp'), may hold values from -8 to 8
- input_gate_pre: float32 [4, 4096], P('tp', 'sp'), may hold values from -8 to 8
- forget_gate_pre: float32 [4, 4096], P('tp', 'sp'), may hold values from -26 to 26
- residual: bfloat16 [4096, 2048], P(('sp', 'tp')), may hold values from -6 to 6
- out_proj: bfloat16 [2048, 2048], P('tp'), may hold values from -0.125 to 0.125
- mix_gain: float32 [2048], replicated, may hold values from 0.1 to 1.9
- pre_gain: float32 [2048], replicated, may hold values from 0.1 to 1.9
- gate_proj: bfloat16 [2048, 3072], P('sp', 'tp'), may hold values from -0.125 to 0.125
- value_proj: bfloat16 [2048, 3072], P('sp', 'tp'), may hold values from -0.125 to 0.125
- gate_kernel: float32 [3, 3072], P(None, 'tp'), may hold values from -3.5 to 3.5
- value_kernel: float32 [3, 3072], P(None, 'tp'), may hold values from -3.5 to 3.5
- down_proj: bfloat16 [2048, 3072], P('sp', 'tp'), may hold values from -0.109375 to 0.109375
- post_gain: float32 [2048], replicated, may hold values from 0.1 to 1.9
Outputs:
- result: bfloat16 [4096, 2048], P(('sp', 'tp'))
The draws below stay inside these ranges and needn't reach their ends.
All inputs are finite; a program needn't handle non-finite values.
Results may differ from the reference program's by a relative error of at most 0.017.
Values may be sent and summed in bfloat16 or wider, within the bound.
A program may use at most 128 MiB of HBM per device.

```python
import math
import jax
import jax.numpy as jnp
from jax import lax

D = 2048
HEADS = 4
QK = 256
HV = 512
FF = 3072
BLOCK = 64
CONV = 3
TOK_DEV = 512
SEQUENCE_TOKENS = 4096
N_TP = 4


def draw_forget_gate_pre(key, part):
    sequence_lanes = jax.random.split(jax.random.fold_in(key, 7301), 6)
    order = jax.random.permutation(sequence_lanes[0], HEADS)
    slow_count = HEADS // 2
    sluggish_decay = (order < slow_count)[:, None]
    spans = SEQUENCE_TOKENS // TOK_DEV
    factor = jnp.exp(jax.random.uniform(sequence_lanes[1], (HEADS, spans), jnp.float32, math.log(0.15), math.log(0.5)))
    factor = jnp.repeat(factor, TOK_DEV, axis=1)
    slow_rate = factor * (math.log(10.0) / SEQUENCE_TOKENS)
    fast_rate = jnp.exp(-jax.random.uniform(sequence_lanes[2], (HEADS, 1), jnp.float32, math.log(8.0), math.log(40.0)))
    rate = jnp.where(sluggish_decay, slow_rate, fast_rate)
    noise = 0.7 * jax.random.normal(sequence_lanes[3], (HEADS, SEQUENCE_TOKENS), jnp.float32)
    magnitude_value = -jnp.log(rate) + noise
    spike_locations = jax.random.randint(sequence_lanes[4], (4,), 0, SEQUENCE_TOKENS)
    spiked_entries = jnp.any(jnp.arange(SEQUENCE_TOKENS)[None, :] == spike_locations[:, None], axis=0)[None, :]
    retained_entries = jax.random.uniform(sequence_lanes[5], (HEADS, SEQUENCE_TOKENS), jnp.float32, 0.5, 0.8)
    spike_height = jnp.log(retained_entries / (1.0 - retained_entries))
    magnitude_value = jnp.where(spiked_entries & sluggish_decay, spike_height, magnitude_value)
    magnitude_value = jnp.clip(magnitude_value, -14.0, 14.0)
    ratio = magnitude_value / 15.0
    return 7.5 * jnp.log((1.0 + ratio) / (1.0 - ratio))


def steps_of(rng, extent, cuts, least, high):
    loudness = 1.0
    for dim, parts in cuts:
        draws = jax.random.uniform(jax.random.fold_in(jax.random.fold_in(rng, 6), dim), (parts,), jnp.float32, least / len(cuts), high / len(cuts))
        loudness = loudness * jnp.repeat(jnp.exp(draws), extent[dim] // parts).reshape((-1,) + (1,) * (len(extent) - 1 - dim))
    return loudness


def scatter_about(rng, extent, deviation, reach, pieces=(), kind=jnp.bfloat16):
    drawn = jax.random.normal(rng, extent, jnp.float32) * deviation
    if len(pieces) > 0:
        drawn = steps_of(rng, extent, pieces, -0.22, 0.18) * drawn
    return jnp.clip(drawn, min=-reach, max=reach).astype(kind)


def setup_inputs(seed: int = 0) -> dict:
    splits = jax.random.split(jax.random.key(seed), 17)
    query_rows = scatter_about(splits[0], (SEQUENCE_TOKENS, HEADS * QK), 1.0, 6.0, ((0, 8), (1, 4)))
    key_rows = scatter_about(splits[1], (SEQUENCE_TOKENS, HEADS * QK), 1.0, 6.0, ((0, 8), (1, 4)))
    value_rows = scatter_about(splits[2], (SEQUENCE_TOKENS, HEADS * HV), 1.0, 6.0, ((0, 8), (1, 4)))
    out_gate_pre = scatter_about(splits[3], (SEQUENCE_TOKENS, HEADS * HV), 1.5, 8.0, ((0, 8), (1, 4)))
    input_gate_pre = scatter_about(splits[4], (HEADS, SEQUENCE_TOKENS), 2.0, 8.0, ((0, 4), (1, 8)), jnp.float32)
    forget_gate_pre = draw_forget_gate_pre(jax.random.fold_in(splits[16], 71), 0)
    residual = scatter_about(splits[6], (SEQUENCE_TOKENS, D), 1.0, 6.0, ((0, 32),))
    out_proj = scatter_about(splits[7], (HEADS * HV, D), (HEADS * HV) ** -0.5, 0.125, ((0, 4),))
    mix_gain = jnp.clip(1.0 + 0.18 * jax.random.normal(splits[8], (D,), jnp.float32), 0.1, 1.9)
    pre_gain = jnp.clip(1.0 + 0.18 * jax.random.normal(splits[9], (D,), jnp.float32), 0.1, 1.9)
    gate_proj = scatter_about(splits[10], (D, FF), D ** -0.5, 0.125, ((0, 8), (1, 4)))
    value_proj = scatter_about(splits[11], (D, FF), D ** -0.5, 0.125, ((0, 8), (1, 4)))
    gate_kernel = scatter_about(splits[12], (CONV, FF), CONV ** -0.5, 3.5, ((1, 4),), jnp.float32)
    value_kernel = scatter_about(splits[13], (CONV, FF), CONV ** -0.5, 3.5, ((1, 4),), jnp.float32)
    down_proj = scatter_about(splits[14], (D, FF), FF ** -0.5, 0.109375, ((0, 8), (1, 4)))
    post_gain = jnp.clip(1.0 + 0.18 * jax.random.normal(splits[15], (D,), jnp.float32), 0.1, 1.9)
    return {"query_rows": query_rows, "key_rows": key_rows, "value_rows": value_rows, "out_gate_pre": out_gate_pre, "input_gate_pre": input_gate_pre, "forget_gate_pre": forget_gate_pre, "residual": residual, "out_proj": out_proj, "mix_gain": mix_gain, "pre_gain": pre_gain, "gate_proj": gate_proj, "value_proj": value_proj, "gate_kernel": gate_kernel, "value_kernel": value_kernel, "down_proj": down_proj, "post_gain": post_gain}


gate_cap = 15.0
epsilon = 1e-06
highest = lax.Precision.HIGHEST

def softcap(values):
    return gate_cap * jnp.tanh(values / gate_cap)

def normalize(values, gains):
    return values * lax.rsqrt(lax.optimization_barrier(jnp.mean(values * values, axis=-1, keepdims=True)) + epsilon) * gains

def barrier_round(values):
    rounded = lax.optimization_barrier(values.astype(jnp.bfloat16))
    return rounded.astype(jnp.float32)

def head_cells(inputs):
    queries, key_heads, value_heads, log_input, log_forget = inputs
    nblocks = SEQUENCE_TOKENS // BLOCK
    causal = jnp.tril(jnp.ones((BLOCK, BLOCK), dtype=bool))

    def advance(carried_state, block_inputs):
        memory, normer, stabilizer = carried_state
        query_blk, key_blk, value_blk, input_blk, forget_blk = block_inputs
        running = jnp.cumsum(forget_blk)
        block_total = running[-1]
        log_weights = jnp.where(causal, running[:, None] - running[None, :] + input_blk[None, :], -jnp.inf)
        carried = running + stabilizer
        row_max = jnp.maximum(carried, lax.optimization_barrier(jnp.max(log_weights, axis=1)))
        inner_weights = jnp.exp(log_weights - row_max[:, None])
        outer_weights = jnp.exp(carried - row_max)
        scores = jnp.dot(query_blk, key_blk.T, precision=highest) * inner_weights
        numerator = outer_weights[:, None] * jnp.dot(query_blk, memory, precision=highest) + jnp.dot(scores, value_blk, precision=highest)
        denominator = outer_weights * jnp.dot(query_blk, normer, precision=highest) + lax.optimization_barrier(jnp.sum(scores, axis=1))
        cell_rows = numerator / jnp.maximum(jnp.abs(denominator), jnp.exp(-row_max))[:, None]
        lead_logs = block_total - running + input_blk
        new_stabilizer = jnp.maximum(block_total + stabilizer, jnp.max(lead_logs))
        lead_weights = jnp.exp(lead_logs - new_stabilizer)
        decay_factor = jnp.exp(block_total + stabilizer - new_stabilizer)
        weighted = key_blk * lead_weights[:, None]
        memory = decay_factor * memory + jnp.dot(weighted.T, value_blk, precision=highest)
        normer = decay_factor * normer + lax.optimization_barrier(jnp.sum(weighted, axis=0))
        return ((memory, normer, new_stabilizer), cell_rows)
    initial = (jnp.zeros((QK, HV), jnp.float32), jnp.zeros((QK,), jnp.float32), jnp.zeros((), jnp.float32))
    stacked = (queries.reshape(nblocks, BLOCK, QK), key_heads.reshape(nblocks, BLOCK, QK), value_heads.reshape(nblocks, BLOCK, HV), log_input.reshape(nblocks, BLOCK), log_forget.reshape(nblocks, BLOCK))
    ignored, outputs = lax.scan(advance, initial, stacked)
    return outputs.reshape(SEQUENCE_TOKENS, HV)

def grouped_sum(left, right, right_axis):
    group_width = left.shape[1] // N_TP
    summed = jnp.zeros((left.shape[0], right.shape[1 - right_axis]), jnp.float32)
    for group_index in range(N_TP):
        left_part = left[:, group_index * group_width:(group_index + 1) * group_width]
        right_part = lax.slice_in_dim(right, group_index * group_width, (group_index + 1) * group_width, axis=right_axis)
        partial_sum = lax.dot_general(left_part, right_part, (((1,), (right_axis,)), ((), ())), preferred_element_type=jnp.float32)
        summed = summed + barrier_round(partial_sum)
    return summed.astype(jnp.bfloat16)

def depthwise(up_rows, kernel):
    length = up_rows.shape[0]
    padded = jnp.pad(up_rows.astype(jnp.float32), ((CONV - 1, 0), (0, 0)))
    summed = kernel[0] * padded[0:length]
    for offset in range(1, CONV):
        summed = summed + kernel[offset] * padded[offset:offset + length]
    return summed

def reference(query_rows, key_rows, value_rows, out_gate_pre, input_gate_pre, forget_gate_pre, residual, out_proj, mix_gain, pre_gain, gate_proj, value_proj, gate_kernel, value_kernel, down_proj, post_gain):
    query_scale = QK ** (-0.5)
    queries = query_rows.astype(jnp.float32).reshape(SEQUENCE_TOKENS, HEADS, QK).transpose(1, 0, 2) * query_scale
    key_heads = key_rows.astype(jnp.float32).reshape(SEQUENCE_TOKENS, HEADS, QK).transpose(1, 0, 2)
    value_heads = value_rows.astype(jnp.float32).reshape(SEQUENCE_TOKENS, HEADS, HV).transpose(1, 0, 2)
    log_input = softcap(input_gate_pre)
    log_forget = jax.nn.log_sigmoid(softcap(forget_gate_pre))
    cell_rows = lax.map(head_cells, (queries, key_heads, value_heads, log_input, log_forget))
    cell_rows = cell_rows.transpose(1, 0, 2).reshape(SEQUENCE_TOKENS, HEADS * HV)
    gated = (cell_rows * jax.nn.sigmoid(out_gate_pre.astype(jnp.float32))).astype(jnp.bfloat16)
    mixed = grouped_sum(gated, out_proj, 0)
    stream = (residual.astype(jnp.float32) + normalize(mixed.astype(jnp.float32), mix_gain)).astype(jnp.bfloat16)
    normed = normalize(stream.astype(jnp.float32), pre_gain).astype(jnp.bfloat16)
    up_gate = jnp.dot(normed, gate_proj, preferred_element_type=jnp.float32).astype(jnp.bfloat16)
    up_value = jnp.dot(normed, value_proj, preferred_element_type=jnp.float32).astype(jnp.bfloat16)
    hidden = (jax.nn.silu(depthwise(up_gate, gate_kernel)) * depthwise(up_value, value_kernel)).astype(jnp.bfloat16)
    ffn = grouped_sum(hidden, down_proj, 1)
    return (stream.astype(jnp.float32) + normalize(ffn.astype(jnp.float32), post_gain)).astype(jnp.bfloat16)
```

```python
import functools
import jax
import jax.numpy as jnp
from jax import lax
from jax.experimental import pallas as pl
from jax.experimental.pallas import tpu as pltpu
from jax.sharding import PartitionSpec as P

CONV = 3
HALO = 16
gate_cap = 15.0
epsilon = 1e-06
far_below = -1e30
MESH = pl.DeviceIdType.MESH
f32 = jnp.float32
bf16 = jnp.bfloat16


def softcap(values):
    return gate_cap * jnp.tanh(values / gate_cap)


def sigmoid(values):
    return 1.0 / (1.0 + jnp.exp(-values))


def normalize(values, gains):
    return values * lax.rsqrt(jnp.mean(values * values, axis=-1, keepdims=True) + epsilon) * gains


def dot(a, b, ca=1, cb=0):
    return lax.dot_general(a, b, (((ca,), (cb,)), ((), ())), preferred_element_type=f32)


def kernel(
    n, m, owners, chunks,
    q_ref, k_ref, v_ref, og_ref, ig_ref, fg_ref, res_ref, op_ref,
    mg_ref, pg_ref, gp_ref, vp_ref, gk_ref, vk_ref, dp_ref, sg_ref,
    out_ref,
    w_all, st_send, small, slices, pre_send, mem_in,
    gated, mix_send, mix_recv, normed_all, upg, upv, halo_send, halo_recv, hidden, ffn_send, ffn_recv,
    own_sem, z_send, x_send, w_recv, sm_send, sm_recv, sl_send, sl_recv, pr_send, pr_recv,
    mx_send, mx_recv, ag_send, ag_recv, h_send, h_recv, f_send, f_recv,
):
    s = lax.axis_index("sp")
    t = lax.axis_index("tp")
    inner = 2
    zs = n // inner
    x = lax.rem(s, inner)
    z = lax.div(s, inner)
    mate = z * inner + (1 - x)
    rows, qk = q_ref.shape
    block = gp_ref.shape[0]
    width = w_all.shape[1]
    part = rows // m
    piece = qk // owners
    scale = qk ** (-0.5)

    def remote(src, dst, ss, rs, **dev):
        return pltpu.make_async_remote_copy(
            src_ref=src, dst_ref=dst, send_sem=ss, recv_sem=rs, device_id=dev, device_id_type=MESH
        )

    barrier = pltpu.get_barrier_semaphore()
    for d in range(1, n):
        pl.semaphore_signal(barrier, inc=1, device_id={"sp": lax.rem(s + d, n)}, device_id_type=MESH)
    for d in range(1, m):
        pl.semaphore_signal(barrier, inc=1, device_id={"tp": lax.rem(t + d, m)}, device_id_type=MESH)
    pl.semaphore_wait(barrier, n + m - 2)

    def slot(w, blk):
        return w_all.at[w, pl.ds(pl.multiple_of(blk * block, block), block), :]

    waits = []
    own = []
    for w, ref in enumerate((gp_ref, vp_ref, dp_ref)):
        c = pltpu.make_async_copy(ref, slot(w, s), own_sem.at[w])
        c.start()
        own.append(c)
        c = remote(ref, slot(w, s), x_send.at[w, 0], w_recv.at[w, s], sp=mate)
        c.start()
        waits.append(c)
        for d in range(1, zs):
            c = remote(
                ref, slot(w, s), z_send.at[w, d - 1], w_recv.at[w, s],
                sp=lax.rem(z + d, zs) * inner + x,
            )
            c.start()
            waits.append(c)

    def arrived(w, blk):
        remote(slot(w, blk), slot(w, blk), x_send.at[w, 0], w_recv.at[w, blk], sp=mate).wait_recv()

    def relay(w, d):
        blk = lax.rem(z + d, zs) * inner + x
        arrived(w, blk)
        c = remote(slot(w, blk), slot(w, blk), x_send.at[w, d], w_recv.at[w, blk], sp=mate)
        c.start()
        waits.append(c)
        return blk

    def mate_block(d):
        return lax.rem(z + d, zs) * inner + (1 - x)

    i = lax.broadcasted_iota(jnp.int32, (rows, rows), 0)
    j = lax.broadcasted_iota(jnp.int32, (rows, rows), 1)
    li_row = softcap(ig_ref[...])
    fg = softcap(fg_ref[...])
    lf_row = jnp.minimum(fg, 0.0) - jnp.log1p(jnp.exp(-jnp.abs(fg)))
    run_col = jnp.sum(jnp.where(j <= i, lf_row, 0.0), axis=1, keepdims=True)
    run_row = jnp.sum(jnp.where(j == i, run_col, 0.0), axis=0, keepdims=True)
    li_col = jnp.sum(jnp.where(j == i, li_row, 0.0), axis=1, keepdims=True)
    total = run_col[rows - 1 : rows, :]
    lead = total - run_col + li_col
    lead_max = jnp.max(lead, axis=0, keepdims=True)
    weighted = k_ref[...].astype(f32) * jnp.exp(lead - lead_max)
    norm_row = jnp.sum(weighted, axis=0, keepdims=True)
    st_send[...] = dot(weighted.astype(bf16), v_ref[...], 0, 0).astype(bf16)
    r8 = lax.broadcasted_iota(jnp.int32, (8, qk), 0)
    small[s] = jnp.where(r8 == 0, norm_row, jnp.where(r8 == 1, total, lead_max))

    def only_owner(who, fn):
        if owners == n:
            fn()
        else:
            pl.when(who < owners)(fn)

    def rows_of(r):
        return pl.ds(pl.multiple_of(r * piece, piece), piece)

    for d in range(1, n):
        to = lax.rem(s + d, n)
        c = remote(small.at[s], small.at[s], sm_send.at[d - 1], sm_recv.at[s], sp=to)
        c.start()
        waits.append(c)

        def send_slice(d=d, to=to):
            remote(
                st_send.at[rows_of(to), :], slices.at[s], sl_send.at[d - 1], sl_recv.at[s], sp=to
            ).start()

        only_owner(to, send_slice)

    def keep_slice():
        slices[s] = st_send[rows_of(s), :]

    only_owner(s, keep_slice)

    log_w = jnp.where(j <= i, run_col - run_row + li_row, far_below)
    loc_max = jnp.max(log_w, axis=1, keepdims=True)
    scores = dot(q_ref[...], k_ref[...], 1, 1) * scale * jnp.exp(log_w - loc_max)
    den_loc = jnp.sum(scores, axis=1, keepdims=True)
    num_loc = dot(scores.astype(bf16), v_ref[...])

    for d in range(1, n):
        src = lax.rem(s + d, n)
        remote(small.at[src], small.at[src], sm_send.at[0], sm_recv.at[src], sp=src).wait_recv()

    def step_small(a, carry):
        top, nrm = carry
        tile = small[a]
        nt = tile[1:2, 0:1] + top
        new = jnp.maximum(nt, tile[2:3, 0:1])
        upd = jnp.exp(nt - new) * nrm + jnp.exp(tile[2:3, 0:1] - new) * tile[0:1, :]
        live = a < s
        return jnp.where(live, new, top), jnp.where(live, upd, nrm)

    def step_mem(a, carry):
        top, mem = carry
        tile = small[a]
        nt = tile[1:2, 0:1] + top
        new = jnp.maximum(nt, tile[2:3, 0:1])
        mem = jnp.exp(nt - new) * mem + jnp.exp(tile[2:3, 0:1] - new) * slices[a].astype(f32)
        pre_send[a + 1] = mem.astype(bf16)
        return new, mem

    def steps(count, fn, carry):
        if count <= 8:
            for a in range(count):
                carry = fn(a, carry)
            return carry
        return lax.fori_loop(0, count, fn, carry)

    start_max = jnp.full((1, 1), far_below, f32)
    m_in, n_in = steps(n - 1, step_small, (start_max, jnp.zeros((1, qk), f32)))

    def own_prefixes():
        for d in range(1, n):
            src = lax.rem(s + d, n)
            remote(
                slices.at[src], slices.at[src], sl_send.at[0], sl_recv.at[src], sp=src
            ).wait_recv()
        pre_send[0] = jnp.zeros(pre_send.shape[1:], bf16)
        steps(n - 1, step_mem, (start_max, jnp.zeros(pre_send.shape[1:], f32)))
        for d in range(1, n):
            to = lax.rem(s + d, n)
            remote(
                pre_send.at[to], mem_in.at[rows_of(s), :], pr_send.at[d - 1], pr_recv.at[s], sp=to
            ).start()
        mem_in[rows_of(s), :] = pre_send[s]

    only_owner(s, own_prefixes)
    for d in range(1, n):
        src = lax.rem(s + d, n)

        def got(src=src):
            remote(
                mem_in.at[rows_of(src), :], mem_in.at[rows_of(src), :],
                pr_send.at[0], pr_recv.at[src], sp=src,
            ).wait_recv()

        only_owner(src, got)

    carried = run_col + m_in
    top = jnp.maximum(carried, loc_max)
    inner_w = jnp.exp(loc_max - top)
    outer_w = jnp.exp(carried - top) * scale
    num = inner_w * num_loc + outer_w * dot(q_ref[...], mem_in[...])
    den = inner_w * den_loc + outer_w * jnp.sum(
        q_ref[...].astype(f32) * n_in, axis=1, keepdims=True
    )
    cell = num / jnp.maximum(jnp.abs(den), jnp.exp(-top))
    gated[...] = (cell * sigmoid(og_ref[...].astype(f32))).astype(bf16)

    def part_of(a):
        return pl.ds(pl.multiple_of(a * part, part), part)

    for d in range(1, m):
        to = lax.rem(t + d, m)
        mix_send[d - 1] = dot(gated[part_of(to), :], op_ref[...]).astype(bf16)
        c = remote(mix_send.at[d - 1], mix_recv.at[d - 1], mx_send.at[d - 1], mx_recv.at[d - 1], tp=to)
        c.start()
        waits.append(c)
    mixed = dot(gated[part_of(t), :], op_ref[...]).astype(bf16).astype(f32)
    for d in range(1, zs):
        relay(0, d)
    for d in range(1, m):
        remote(
            mix_send.at[d - 1], mix_recv.at[d - 1], mx_send.at[d - 1], mx_recv.at[d - 1], tp=t
        ).wait_recv()
        mixed = mixed + mix_recv[d - 1].astype(f32)
    mixed = mixed.astype(bf16).astype(f32)
    stream = (res_ref[...].astype(f32) + normalize(mixed, mg_ref[...])).astype(bf16)
    out_ref[...] = stream
    normed_all[part_of(t), :] = normalize(stream.astype(f32), pg_ref[...]).astype(bf16)
    for d in range(1, m):
        to = lax.rem(t + d, m)
        c = remote(
            normed_all.at[part_of(t), :], normed_all.at[part_of(t), :],
            ag_send.at[d - 1], ag_recv.at[t], tp=to,
        )
        c.start()
        waits.append(c)
    for d in range(1, zs):
        relay(1, d)
    own[0].wait()
    own[1].wait()
    for w in range(2):
        for d in range(zs):
            arrived(w, mate_block(d))
    for d in range(1, m):
        src = lax.rem(t + d, m)
        remote(
            normed_all.at[part_of(src), :], normed_all.at[part_of(src), :],
            ag_send.at[0], ag_recv.at[src], tp=src,
        ).wait_recv()

    hid = upg.shape[1]
    cols = 256 if hid % 256 == 0 else 128
    for w, ref in ((0, upg), (1, upv)):

        def up_cols(a, _, w=w, ref=ref):
            cs = pl.ds(pl.multiple_of(a * cols, cols), cols)
            ref[pl.ds(HALO, rows), cs] = dot(normed_all[...], w_all[w, :, cs]).astype(bf16)
            return 0

        lax.fori_loop(0, hid // cols, up_cols, 0)
        halo_send[w] = ref[pl.ds(rows, HALO), :]

    halo = remote(halo_send, halo_recv, h_send, h_recv, sp=lax.rem(s + 1, n))

    @pl.when(s < n - 1)
    def _():
        halo.start()

    @pl.when(s == 0)
    def _():
        upg[pl.ds(0, HALO), :] = jnp.zeros((HALO, hid), bf16)
        upv[pl.ds(0, HALO), :] = jnp.zeros((HALO, hid), bf16)

    @pl.when(s > 0)
    def _():
        halo.wait_recv()
        upg[pl.ds(0, HALO), :] = halo_recv[0]
        upv[pl.ds(0, HALO), :] = halo_recv[1]

    def conv(ref, kern, r0, cs):
        u = ref[pl.ds(r0, part + HALO), cs].astype(f32)
        total_ = kern[CONV - 1 : CONV, cs] * u
        for back in range(1, CONV):
            total_ = total_ + kern[CONV - 1 - back : CONV - back, cs] * pltpu.roll(u, back, 0)
        return total_[HALO:, :]

    def conv_rows(a, _):
        r0 = pl.multiple_of(a * part, part)
        for c0 in range(0, hid, cols):
            cs = pl.ds(c0, cols)
            g = conv(upg, gk_ref, r0, cs)
            u = conv(upv, vk_ref, r0, cs)
            hidden[pl.ds(r0, part), cs] = (g / (1.0 + jnp.exp(-g)) * u).astype(bf16)
        return 0

    lax.fori_loop(0, rows // part, conv_rows, 0)

    feats = width // chunks

    def chunk(c, kth):
        fs = pl.ds(pl.multiple_of(c * feats, feats), feats)
        ffn_send[:, fs] = dot(hidden[...], w_all[2, fs, :], 1, 1).astype(bf16)
        for d in range(1, m):
            to = lax.rem(t + d, m)
            cp = remote(
                ffn_send.at[part_of(to), fs], ffn_recv.at[d - 1, :, fs],
                f_send.at[d - 1, kth], f_recv.at[d - 1, c], tp=to,
            )
            cp.start()
            waits.append(cp)

    own[2].wait()
    if chunks == n:
        chunk(s, 0)
        for d in range(1, zs):
            chunk(relay(2, d), d)
        for d in range(zs):
            blk = mate_block(d)
            arrived(2, blk)
            chunk(blk, zs + d)
    else:
        for d in range(1, zs):
            relay(2, d)
        for d in range(zs):
            arrived(2, mate_block(d))
        for c in range(chunks):
            chunk(c, c)

    for c in range(chunks):
        fs = pl.ds(c * feats, feats)
        for d in range(1, m):
            remote(
                ffn_send.at[part_of(t), fs], ffn_recv.at[d - 1, :, fs],
                f_send.at[d - 1, 0], f_recv.at[d - 1, c], tp=t,
            ).wait_recv()
    ffn = ffn_send[part_of(t), :].astype(f32)
    for d in range(1, m):
        ffn = ffn + ffn_recv[d - 1].astype(f32)
    ffn = ffn.astype(bf16).astype(f32)
    out_ref[...] = (out_ref[...].astype(f32) + normalize(ffn, sg_ref[...])).astype(bf16)

    for c in waits:
        c.wait_send()
    for d in range(1, n):
        to = lax.rem(s + d, n)

        def done_slice(d=d, to=to):
            remote(
                st_send.at[rows_of(to), :], slices.at[s], sl_send.at[d - 1], sl_recv.at[s], sp=to
            ).wait_send()

        only_owner(to, done_slice)

    def done_prefix():
        for d in range(1, n):
            to = lax.rem(s + d, n)
            remote(
                pre_send.at[to], mem_in.at[rows_of(s), :], pr_send.at[d - 1], pr_recv.at[s], sp=to
            ).wait_send()

    only_owner(s, done_prefix)

    @pl.when(s < n - 1)
    def _():
        halo.wait_send()


def body(
    n, m,
    query_rows, key_rows, value_rows, out_gate_pre, input_gate_pre, forget_gate_pre,
    residual, out_proj, mix_gain, pre_gain, gate_proj, value_proj, gate_kernel, value_kernel,
    down_proj, post_gain,
):
    rows, qk = query_rows.shape
    hv = value_rows.shape[1]
    width = residual.shape[1]
    block, hid = gate_proj.shape
    part = rows // m
    owners = min(n, qk // 32)
    chunks = min(n, width // 256)
    dma = pltpu.SemaphoreType.DMA
    vm = pl.BlockSpec(memory_space=pltpu.VMEM)
    hbm = pl.BlockSpec(memory_space=pl.ANY)
    zs = n // 2
    return pl.pallas_call(
        functools.partial(kernel, n, m, owners, chunks),
        out_shape=jax.ShapeDtypeStruct(residual.shape, bf16),
        in_specs=[vm] * 10 + [hbm, hbm, vm, vm, hbm, vm],
        out_specs=vm,
        scratch_shapes=[
            pltpu.VMEM((3, width, hid), bf16),
            pltpu.VMEM((qk, hv), bf16),
            pltpu.VMEM((n, 8, qk), f32),
            pltpu.VMEM((n, qk // owners, hv), bf16),
            pltpu.VMEM((n, qk // owners, hv), bf16),
            pltpu.VMEM((qk, hv), bf16),
            pltpu.VMEM((rows, hv), bf16),
            pltpu.VMEM((m - 1, part, width), bf16),
            pltpu.VMEM((m - 1, part, width), bf16),
            pltpu.VMEM((rows, width), bf16),
            pltpu.VMEM((HALO + rows, hid), bf16),
            pltpu.VMEM((HALO + rows, hid), bf16),
            pltpu.VMEM((2, HALO, hid), bf16),
            pltpu.VMEM((2, HALO, hid), bf16),
            pltpu.VMEM((rows, hid), bf16),
            pltpu.VMEM((rows, width), bf16),
            pltpu.VMEM((m - 1, part, width), bf16),
            dma((3,)),
            dma((3, zs)),
            dma((3, zs)),
            dma((3, n)),
            dma((n,)),
            dma((n,)),
            dma((n,)),
            dma((n,)),
            dma((n,)),
            dma((n,)),
            dma((m,)),
            dma((m,)),
            dma((m,)),
            dma((m,)),
            dma,
            dma,
            dma((m, chunks)),
            dma((m, chunks)),
        ],
        compiler_params=pltpu.CompilerParams(
            collective_id=0, has_side_effects=True, vmem_limit_bytes=64000000
        ),
        name="layer",
    )(
        query_rows, key_rows, value_rows, out_gate_pre, input_gate_pre, forget_gate_pre,
        residual, out_proj, mix_gain.reshape(1, -1), pre_gain.reshape(1, -1),
        gate_proj, value_proj, gate_kernel, value_kernel, down_proj, post_gain.reshape(1, -1),
    )


def solution(mesh):
    return jax.shard_map(
        functools.partial(body, mesh.shape["sp"], mesh.shape["tp"]),
        mesh=mesh,
        in_specs=(
            P("sp", "tp"),
            P("sp", "tp"),
            P("sp", "tp"),
            P("sp", "tp"),
            P("tp", "sp"),
            P("tp", "sp"),
            P(("sp", "tp"), None),
            P("tp", None),
            P(),
            P(),
            P("sp", "tp"),
            P("sp", "tp"),
            P(None, "tp"),
            P(None, "tp"),
            P("sp", "tp"),
            P(),
        ),
        out_specs=P(("sp", "tp"), None),
        check_vma=False,
    )
```

```python
import functools
import jax
import jax.numpy as jnp
from jax import lax
from jax.experimental import pallas as pl
from jax.experimental.pallas import tpu as pltpu
from jax.sharding import PartitionSpec as P

CONV = 3
HALO = 16
gate_cap = 15.0
epsilon = 1e-06
far_below = -1e30
MESH = pl.DeviceIdType.MESH
f32 = jnp.float32
bf16 = jnp.bfloat16


def softcap(values):
    return gate_cap * jnp.tanh(values / gate_cap)


def sigmoid(values):
    return 1.0 / (1.0 + jnp.exp(-values))


def normalize(values, gains):
    return values * lax.rsqrt(jnp.mean(values * values, axis=-1, keepdims=True) + epsilon) * gains


def dot(a, b, ca=1, cb=0):
    return lax.dot_general(a, b, (((ca,), (cb,)), ((), ())), preferred_element_type=f32)


def kernel(
    n, m, owners, chunks,
    q_ref, k_ref, v_ref, og_ref, ig_ref, fg_ref, res_ref, op_ref,
    mg_ref, pg_ref, gp_ref, vp_ref, gk_ref, vk_ref, dp_ref, sg_ref,
    out_ref,
    w_all, st_send, small, slices, pre_send, mem_in,
    gated, mix_send, mix_pair, mix_far, mix_recv, normed_all, upg, upv, halo_send, halo_recv, hidden, ffn_send, ffn_pair, ffn_far, ffn_recv,
    own_sem, z_send, x_send, w_recv, sm_send, sm_recv, sl_send, sl_recv, pr_send, pr_recv,
    mx_send, mx_recv, my_send, my_recv, ag_send, ag_recv, h_send, h_recv, f_send, f_recv, g_send, g_recv,
):
    s = lax.axis_index("sp")
    t = lax.axis_index("tp")
    inner = 2
    zs = n // inner
    x = lax.rem(s, inner)
    z = lax.div(s, inner)
    mate = z * inner + (1 - x)
    rows, qk = q_ref.shape
    block = gp_ref.shape[0]
    width = w_all.shape[1]
    part = rows // m
    piece = qk // owners
    scale = qk ** (-0.5)

    def remote(src, dst, ss, rs, **dev):
        return pltpu.make_async_remote_copy(
            src_ref=src, dst_ref=dst, send_sem=ss, recv_sem=rs, device_id=dev, device_id_type=MESH
        )

    barrier = pltpu.get_barrier_semaphore()
    for d in range(1, n):
        pl.semaphore_signal(barrier, inc=1, device_id={"sp": lax.rem(s + d, n)}, device_id_type=MESH)
    for d in range(1, m):
        pl.semaphore_signal(barrier, inc=1, device_id={"tp": lax.rem(t + d, m)}, device_id_type=MESH)
    pl.semaphore_wait(barrier, n + m - 2)

    def slot(w, blk):
        return w_all.at[w, pl.ds(pl.multiple_of(blk * block, block), block), :]

    waits = []
    held = []
    own = []
    refs = (gp_ref, vp_ref, dp_ref)
    above = jnp.minimum(z + 1, zs - 1) * inner + x
    below = jnp.maximum(z - 1, 0) * inner + x
    has_above = z + 1 < zs
    has_below = z > 0

    def pass_on(w, src, blk, k, cond, to):
        c = remote(src, slot(w, blk), z_send.at[w, k], w_recv.at[w, blk], sp=to)
        pl.when(cond)(c.start)
        held.append((cond, c))

    def send_own(w):
        pass_on(w, refs[w], s, 0, has_above, above)
        pass_on(w, refs[w], s, zs, has_below, below)
        c = remote(refs[w], slot(w, s), x_send.at[w, 0], w_recv.at[w, s], sp=mate)
        c.start()
        waits.append(c)
        c = pltpu.make_async_copy(refs[w], slot(w, s), own_sem.at[w])
        c.start()
        own.append(c)

    def arrived(w, blk):
        remote(slot(w, blk), slot(w, blk), x_send.at[w, 0], w_recv.at[w, blk], sp=mate).wait_recv()

    def relay_one(w, k, upward):
        if upward:
            cond, zz, room, to, base = z >= k, jnp.maximum(z - k, 0), has_above, above, 0
        else:
            cond, zz, room, to, base = z + k < zs, jnp.minimum(z + k, zs - 1), has_below, below, zs
        blk = zz * inner + x

        @pl.when(cond)
        def _():
            arrived(w, blk)

        if k < zs - 1:
            pass_on(w, slot(w, blk), blk, base + k, jnp.logical_and(cond, room), to)
        c = remote(slot(w, blk), slot(w, blk), x_send.at[w, base + k], w_recv.at[w, blk], sp=mate)
        pl.when(cond)(c.start)
        held.append((cond, c))

    def relay(w, k):
        relay_one(w, k, True)
        relay_one(w, k, False)

    turn = 1 - 2 * (z // max(zs // 2, 1))

    def column(d, side):
        return lax.rem(z + turn * d + zs, zs) * inner + side

    send_own(0)
    send_own(1)

    i = lax.broadcasted_iota(jnp.int32, (rows, rows), 0)
    j = lax.broadcasted_iota(jnp.int32, (rows, rows), 1)
    li_row = softcap(ig_ref[...])
    fg = softcap(fg_ref[...])
    lf_row = jnp.minimum(fg, 0.0) - jnp.log1p(jnp.exp(-jnp.abs(fg)))
    run_col = jnp.sum(jnp.where(j <= i, lf_row, 0.0), axis=1, keepdims=True)
    run_row = jnp.sum(jnp.where(j == i, run_col, 0.0), axis=0, keepdims=True)
    li_col = jnp.sum(jnp.where(j == i, li_row, 0.0), axis=1, keepdims=True)
    total = run_col[rows - 1 : rows, :]
    lead = total - run_col + li_col
    lead_max = jnp.max(lead, axis=0, keepdims=True)
    weighted = k_ref[...].astype(f32) * jnp.exp(lead - lead_max)
    norm_row = jnp.sum(weighted, axis=0, keepdims=True)
    st_send[...] = dot(weighted.astype(bf16), v_ref[...], 0, 0).astype(bf16)
    r8 = lax.broadcasted_iota(jnp.int32, (8, qk), 0)
    small[s] = jnp.where(r8 == 0, norm_row, jnp.where(r8 == 1, total, lead_max))

    def only_owner(who, fn):
        if owners == n:
            fn()
        else:
            pl.when(who < owners)(fn)

    def rows_of(r):
        return pl.ds(pl.multiple_of(r * piece, piece), piece)

    for d in range(1, n):
        to = lax.rem(s + d, n)
        c = remote(small.at[s], small.at[s], sm_send.at[d - 1], sm_recv.at[s], sp=to)
        c.start()
        waits.append(c)

        def send_slice(d=d, to=to):
            remote(
                st_send.at[rows_of(to), :], slices.at[s], sl_send.at[d - 1], sl_recv.at[s], sp=to
            ).start()

        only_owner(to, send_slice)

    def keep_slice():
        slices[s] = st_send[rows_of(s), :]

    only_owner(s, keep_slice)

    if zs > 1:
        relay(0, 1)
        relay(1, 1)

    log_w = jnp.where(j <= i, run_col - run_row + li_row, far_below)
    loc_max = jnp.max(log_w, axis=1, keepdims=True)
    scores = dot(q_ref[...], k_ref[...], 1, 1) * scale * jnp.exp(log_w - loc_max)
    den_loc = jnp.sum(scores, axis=1, keepdims=True)
    num_loc = dot(scores.astype(bf16), v_ref[...])

    for d in range(1, n):
        src = lax.rem(s + d, n)
        remote(small.at[src], small.at[src], sm_send.at[0], sm_recv.at[src], sp=src).wait_recv()

    def step_small(a, carry):
        top, nrm = carry
        tile = small[a]
        nt = tile[1:2, 0:1] + top
        new = jnp.maximum(nt, tile[2:3, 0:1])
        upd = jnp.exp(nt - new) * nrm + jnp.exp(tile[2:3, 0:1] - new) * tile[0:1, :]
        live = a < s
        return jnp.where(live, new, top), jnp.where(live, upd, nrm)

    def step_mem(a, carry):
        top, mem = carry
        tile = small[a]
        nt = tile[1:2, 0:1] + top
        new = jnp.maximum(nt, tile[2:3, 0:1])
        mem = jnp.exp(nt - new) * mem + jnp.exp(tile[2:3, 0:1] - new) * slices[a].astype(f32)
        pre_send[a + 1] = mem.astype(bf16)
        return new, mem

    def steps(count, fn, carry):
        if count <= 8:
            for a in range(count):
                carry = fn(a, carry)
            return carry
        return lax.fori_loop(0, count, fn, carry)

    start_max = jnp.full((1, 1), far_below, f32)
    m_in, n_in = steps(n - 1, step_small, (start_max, jnp.zeros((1, qk), f32)))

    def own_prefixes():
        for d in range(1, n):
            src = lax.rem(s + d, n)
            remote(
                slices.at[src], slices.at[src], sl_send.at[0], sl_recv.at[src], sp=src
            ).wait_recv()
        pre_send[0] = jnp.zeros(pre_send.shape[1:], bf16)
        steps(n - 1, step_mem, (start_max, jnp.zeros(pre_send.shape[1:], f32)))
        for d in range(1, n):
            to = lax.rem(s + d, n)
            remote(
                pre_send.at[to], mem_in.at[rows_of(s), :], pr_send.at[d - 1], pr_recv.at[s], sp=to
            ).start()
        mem_in[rows_of(s), :] = pre_send[s]

    only_owner(s, own_prefixes)
    for d in range(1, n):
        src = lax.rem(s + d, n)

        def got(src=src):
            remote(
                mem_in.at[rows_of(src), :], mem_in.at[rows_of(src), :],
                pr_send.at[0], pr_recv.at[src], sp=src,
            ).wait_recv()

        only_owner(src, got)

    if zs > 2:
        relay(0, 2)
        relay(1, 2)
    send_own(2)

    carried = run_col + m_in
    top = jnp.maximum(carried, loc_max)
    inner_w = jnp.exp(loc_max - top)
    outer_w = jnp.exp(carried - top) * scale
    num = inner_w * num_loc + outer_w * dot(q_ref[...], mem_in[...])
    den = inner_w * den_loc + outer_w * jnp.sum(
        q_ref[...].astype(f32) * n_in, axis=1, keepdims=True
    )
    cell = num / jnp.maximum(jnp.abs(den), jnp.exp(-top))
    gated[...] = (cell * sigmoid(og_ref[...].astype(f32))).astype(bf16)

    def part_of(a):
        return pl.ds(pl.multiple_of(a * part, part), part)

    c2 = lax.rem(t, 2)
    y = lax.div(t, 2)
    ys = m // 2
    twin = y * 2 + (1 - c2)

    def across(d, side):
        return lax.rem(y + d, ys) * 2 + side

    order = list(range(1, ys)) + [0]
    pair = []
    for d in order:
        mix_send[d] = dot(gated[part_of(across(d, 1 - c2)), :], op_ref[...]).astype(bf16)
        c = remote(mix_send.at[d], mix_pair.at[d], mx_send.at[d], mx_recv.at[d], tp=twin)
        c.start()
        waits.append(c)
        pair.append(c)
    for d, pc in zip(order, pair):
        mixed = dot(gated[part_of(across(d, c2)), :], op_ref[...]).astype(bf16).astype(f32)
        pc.wait_recv()
        mixed = mixed + mix_pair[d].astype(f32)
        if d > 0:
            mix_far[d - 1] = mixed.astype(bf16)
            c = remote(
                mix_far.at[d - 1], mix_recv.at[d - 1], my_send.at[d - 1], my_recv.at[d - 1],
                tp=across(d, c2),
            )
            c.start()
            waits.append(c)
    for k in range(3, zs):
        relay(0, k)
        relay(1, k)
    for d in range(1, ys):
        remote(
            mix_far.at[d - 1], mix_recv.at[d - 1], my_send.at[d - 1], my_recv.at[d - 1], tp=twin
        ).wait_recv()
        mixed = mixed + mix_recv[d - 1].astype(f32)
    mixed = mixed.astype(bf16).astype(f32)
    stream = (res_ref[...].astype(f32) + normalize(mixed, mg_ref[...])).astype(bf16)
    out_ref[...] = stream
    normed_all[part_of(t), :] = normalize(stream.astype(f32), pg_ref[...]).astype(bf16)
    def spread(src, sem, to):
        c = remote(
            normed_all.at[part_of(src), :], normed_all.at[part_of(src), :], sem, ag_recv.at[src], tp=to
        )
        c.start()
        waits.append(c)

    def landed(src):
        remote(
            normed_all.at[part_of(src), :], normed_all.at[part_of(src), :],
            ag_send.at[0], ag_recv.at[src], tp=twin,
        ).wait_recv()

    for d in range(1, ys):
        spread(t, ag_send.at[d], across(d, c2))
    spread(t, ag_send.at[0], twin)
    if zs > 1:
        relay(2, 1)
    for d in range(1, ys):
        landed(across(d, c2))
        spread(across(d, c2), ag_send.at[ys + d], twin)
    for d in range(ys):
        landed(across(d, 1 - c2))
    if zs > 2:
        relay(2, 2)
    own[0].wait()
    own[1].wait()
    for w in range(2):
        for d in range(zs):
            arrived(w, column(d, 1 - x))

    hid = upg.shape[1]
    cols = 256 if hid % 256 == 0 else 128
    for w, ref in ((0, upg), (1, upv)):

        def up_cols(a, _, w=w, ref=ref):
            cs = pl.ds(pl.multiple_of(a * cols, cols), cols)
            ref[pl.ds(HALO, rows), cs] = dot(normed_all[...], w_all[w, :, cs]).astype(bf16)
            return 0

        lax.fori_loop(0, hid // cols, up_cols, 0)
        halo_send[w] = ref[pl.ds(rows, HALO), :]

    halo = remote(halo_send, halo_recv, h_send, h_recv, sp=lax.rem(s + 1, n))

    @pl.when(s < n - 1)
    def _():
        halo.start()

    @pl.when(s == 0)
    def _():
        upg[pl.ds(0, HALO), :] = jnp.zeros((HALO, hid), bf16)
        upv[pl.ds(0, HALO), :] = jnp.zeros((HALO, hid), bf16)

    @pl.when(s > 0)
    def _():
        halo.wait_recv()
        upg[pl.ds(0, HALO), :] = halo_recv[0]
        upv[pl.ds(0, HALO), :] = halo_recv[1]

    def conv(ref, kern, r0, cs):
        u = ref[pl.ds(r0, part + HALO), cs].astype(f32)
        total_ = kern[CONV - 1 : CONV, cs] * u
        for back in range(1, CONV):
            total_ = total_ + kern[CONV - 1 - back : CONV - back, cs] * pltpu.roll(u, back, 0)
        return total_[HALO:, :]

    def conv_rows(a, _):
        r0 = pl.multiple_of(a * part, part)
        for c0 in range(0, hid, cols):
            cs = pl.ds(c0, cols)
            g = conv(upg, gk_ref, r0, cs)
            u = conv(upv, vk_ref, r0, cs)
            hidden[pl.ds(r0, part), cs] = (g / (1.0 + jnp.exp(-g)) * u).astype(bf16)
        return 0

    lax.fori_loop(0, rows // part, conv_rows, 0)

    feats = width // chunks

    def chunk(c, kth):
        fs = pl.ds(pl.multiple_of(c * feats, feats), feats)
        ffn_send[:, fs] = dot(hidden[...], w_all[2, fs, :], 1, 1).astype(bf16)
        for d in order:
            cp = remote(
                ffn_send.at[part_of(across(d, 1 - c2)), fs], ffn_pair.at[d, :, fs],
                f_send.at[d, kth], f_recv.at[d, c], tp=twin,
            )
            cp.start()
            waits.append(cp)

    def paired(c, d):
        fs = pl.ds(pl.multiple_of(c * feats, feats), feats)
        remote(
            ffn_pair.at[d, :, fs], ffn_pair.at[d, :, fs], f_send.at[d, 0], f_recv.at[d, c], tp=twin
        ).wait_recv()

    def far(c, kth):
        fs = pl.ds(pl.multiple_of(c * feats, feats), feats)
        for d in range(1, ys):
            paired(c, d)
            ffn_far[d - 1, :, fs] = (
                ffn_send[part_of(across(d, c2)), fs].astype(f32) + ffn_pair[d, :, fs].astype(f32)
            ).astype(bf16)
            cp = remote(
                ffn_far.at[d - 1, :, fs], ffn_recv.at[d - 1, :, fs],
                g_send.at[d - 1, kth], g_recv.at[d - 1, c], tp=across(d, c2),
            )
            cp.start()
            waits.append(cp)

    for k in range(3, zs):
        relay(2, k)
    own[2].wait()
    ready = []
    if chunks == n:
        for d in range(zs):
            ready.append((column(d, x), False))
        for d in range(zs):
            ready.append((column(d, 1 - x), True))
    else:
        for d in range(zs):
            arrived(2, column(d, 1 - x))
        ready = [(c, False) for c in range(chunks)]
    for kth, (c, late) in enumerate(ready):
        if late:
            arrived(2, c)
        chunk(c, kth)
        if kth > 0:
            far(ready[kth - 1][0], kth - 1)
    far(ready[-1][0], chunks - 1)

    for c in range(chunks):
        fs = pl.ds(c * feats, feats)
        paired(c, 0)
        for d in range(1, ys):
            remote(
                ffn_far.at[d - 1, :, fs], ffn_recv.at[d - 1, :, fs],
                g_send.at[d - 1, 0], g_recv.at[d - 1, c], tp=twin,
            ).wait_recv()
    ffn = ffn_send[part_of(t), :].astype(f32) + ffn_pair[0].astype(f32)
    for d in range(1, ys):
        ffn = ffn + ffn_recv[d - 1].astype(f32)
    ffn = ffn.astype(bf16).astype(f32)
    out_ref[...] = (out_ref[...].astype(f32) + normalize(ffn, sg_ref[...])).astype(bf16)

    for c in waits:
        c.wait_send()
    for cond, c in held:
        pl.when(cond)(c.wait_send)
    for d in range(1, n):
        to = lax.rem(s + d, n)

        def done_slice(d=d, to=to):
            remote(
                st_send.at[rows_of(to), :], slices.at[s], sl_send.at[d - 1], sl_recv.at[s], sp=to
            ).wait_send()

        only_owner(to, done_slice)

    def done_prefix():
        for d in range(1, n):
            to = lax.rem(s + d, n)
            remote(
                pre_send.at[to], mem_in.at[rows_of(s), :], pr_send.at[d - 1], pr_recv.at[s], sp=to
            ).wait_send()

    only_owner(s, done_prefix)

    @pl.when(s < n - 1)
    def _():
        halo.wait_send()


def body(
    n, m,
    query_rows, key_rows, value_rows, out_gate_pre, input_gate_pre, forget_gate_pre,
    residual, out_proj, mix_gain, pre_gain, gate_proj, value_proj, gate_kernel, value_kernel,
    down_proj, post_gain,
):
    rows, qk = query_rows.shape
    hv = value_rows.shape[1]
    width = residual.shape[1]
    block, hid = gate_proj.shape
    part = rows // m
    owners = min(n, qk // 32)
    chunks = min(n, width // 256)
    dma = pltpu.SemaphoreType.DMA
    vm = pl.BlockSpec(memory_space=pltpu.VMEM)
    hbm = pl.BlockSpec(memory_space=pl.ANY)
    zs = n // 2
    ys = m // 2
    return pl.pallas_call(
        functools.partial(kernel, n, m, owners, chunks),
        out_shape=jax.ShapeDtypeStruct(residual.shape, bf16),
        in_specs=[vm] * 10 + [hbm, hbm, vm, vm, hbm, vm],
        out_specs=vm,
        scratch_shapes=[
            pltpu.VMEM((3, width, hid), bf16),
            pltpu.VMEM((qk, hv), bf16),
            pltpu.VMEM((n, 8, qk), f32),
            pltpu.VMEM((n, qk // owners, hv), bf16),
            pltpu.VMEM((n, qk // owners, hv), bf16),
            pltpu.VMEM((qk, hv), bf16),
            pltpu.VMEM((rows, hv), bf16),
            pltpu.VMEM((ys, part, width), bf16),
            pltpu.VMEM((ys, part, width), bf16),
            pltpu.VMEM((ys, part, width), bf16),
            pltpu.VMEM((ys, part, width), bf16),
            pltpu.VMEM((rows, width), bf16),
            pltpu.VMEM((HALO + rows, hid), bf16),
            pltpu.VMEM((HALO + rows, hid), bf16),
            pltpu.VMEM((2, HALO, hid), bf16),
            pltpu.VMEM((2, HALO, hid), bf16),
            pltpu.VMEM((rows, hid), bf16),
            pltpu.VMEM((rows, width), bf16),
            pltpu.VMEM((ys, part, width), bf16),
            pltpu.VMEM((ys, part, width), bf16),
            pltpu.VMEM((ys, part, width), bf16),
            dma((3,)),
            dma((3, 2 * zs)),
            dma((3, 2 * zs)),
            dma((3, n)),
            dma((n,)),
            dma((n,)),
            dma((n,)),
            dma((n,)),
            dma((n,)),
            dma((n,)),
            dma((m,)),
            dma((m,)),
            dma((m,)),
            dma((m,)),
            dma((m,)),
            dma((m,)),
            dma,
            dma,
            dma((ys, chunks)),
            dma((ys, chunks)),
            dma((ys, chunks)),
            dma((ys, chunks)),
        ],
        compiler_params=pltpu.CompilerParams(
            collective_id=0, has_side_effects=True, vmem_limit_bytes=64000000
        ),
        name="layer",
    )(
        query_rows, key_rows, value_rows, out_gate_pre, input_gate_pre, forget_gate_pre,
        residual, out_proj, mix_gain.reshape(1, -1), pre_gain.reshape(1, -1),
        gate_proj, value_proj, gate_kernel, value_kernel, down_proj, post_gain.reshape(1, -1),
    )


def solution(mesh):
    return jax.shard_map(
        functools.partial(body, mesh.shape["sp"], mesh.shape["tp"]),
        mesh=mesh,
        in_specs=(
            P("sp", "tp"),
            P("sp", "tp"),
            P("sp", "tp"),
            P("sp", "tp"),
            P("tp", "sp"),
            P("tp", "sp"),
            P(("sp", "tp"), None),
            P("tp", None),
            P(),
            P(),
            P("sp", "tp"),
            P("sp", "tp"),
            P(None, "tp"),
            P(None, "tp"),
            P("sp", "tp"),
            P(),
        ),
        out_specs=P(("sp", "tp"), None),
        check_vma=False,
    )
```
